512 devices in a mesh: sp: 256 (over z, y, x), tp: 2 (over core).
Axes of the slice: x: 4, y: 8, z: 8, core: 2. Of those that a mesh axis runs over, the one named last changes fastest.
Arguments:
- features: bfloat16 [65536, 1024], P('sp', 'tp'), may hold values from -6 to 6
- lambda_real: float32 [64, 64], P('tp'), may hold values from -4 to 0, as said below
- lambda_imag: float32 [64, 64], P('tp'), may hold values from 0.5 to 201.06177
- log_step: float32 [64], P('tp'), may hold values from -5 to -2
- input_real: float32 [64, 64, 16], P('tp'), may hold values from -0.5 to 0.5
- input_imag: float32 [64, 64, 16], P('tp'), may hold values from -0.5 to 0.5
- real_output: float32 [64, 16, 64], P('tp'), may hold values from -0.75 to 0.75
- imaginary_output: float32 [64, 16, 64], P('tp'), may hold values from -0.75 to 0.75
- skip_gain: float32 [1024], P('tp'), may hold values from -4 to 4
- value_weight: bfloat16 [1024, 2048], P('tp'), may hold values from -0.1875 to 0.1875
- gate_weight: bfloat16 [1024, 2048], P('tp'), may hold values from -0.1875 to 0.1875
- value_bias: float32 [2048], replicated, may hold values from -3 to 3
- gate_bias: float32 [2048], replicated, may hold values from -3 to 3
Outputs:
- mixed_output: bfloat16 [65536, 2048], P(('sp', 'tp'))
The draws below stay inside these ranges and needn't reach their ends.
Inputs may be any that keep to these rules, and one draw needn't show every extreme that they name: `lambda_real`: negative.
All inputs are finite; a program needn't handle non-finite values.
Results may differ from the reference program's by a relative error of at most 0.03.
Values may be sent and summed in bfloat16 or wider, within the bound.
No kernel may reach another device: no remote copies, remote signals or barrier semaphores. Data moves between devices by JAX's collectives and lax.ppermute only.
A program may use at most 128 MiB of HBM per device.

```python
import math
import jax
import jax.numpy as jnp
from jax import lax

D = 2048
CHANNELS = 1024
GROUP = 16
STATE = 64
TOK_SP = 256
GROUPS = 64
LENGTH = 65536
N_TP = 2


def group_rates(key):
    base_key = jax.random.fold_in(key, 91)
    key_flag, key_step, key_rate = jax.random.split(base_key, 3)
    fast_share = 5
    fast_flag = jax.random.randint(key_flag, (GROUPS,), 0, 10) < fast_share
    log_step = jax.random.uniform(key_step, (GROUPS,), jnp.float32, math.log(0.01), math.log(0.1))
    step_size = jnp.exp(log_step)[:, None]
    rate_draw = jax.random.uniform(key_rate, (GROUPS, STATE), jnp.float32, 0.0, 1.0)
    fast_rate = (0.01 + 0.023 * rate_draw) / step_size
    slow_rate = (0.3 + 1.7 * rate_draw) / (LENGTH * step_size)
    lambda_real = -jnp.where(fast_flag[:, None], fast_rate, slow_rate)
    return (lambda_real.astype(jnp.float32), log_step.astype(jnp.float32))


def draw_lambda_real(key, part):
    return group_rates(key)[0]


def draw_log_step(key, part):
    return group_rates(key)[1]


def block_levels(key, dims, cuts, low, top_value):
    loudness = 1.0
    for dim, blocks in cuts:
        draws = jax.random.uniform(jax.random.fold_in(jax.random.fold_in(key, 6), dim), (blocks,), jnp.float32, low / len(cuts), top_value / len(cuts))
        loudness = loudness * jnp.repeat(jnp.exp(draws), dims[dim] // blocks).reshape((-1,) + (1,) * (len(dims) - 1 - dim))
    return loudness


def normal_values(own_key, extent, width, bound, pieces=(), held_as=jnp.bfloat16):
    values = jax.random.normal(own_key, extent, jnp.float32) * width
    if len(pieces) > 0:
        values = block_levels(own_key, extent, pieces, -0.22, 0.18) * values
    return jnp.clip(values, min=-bound, max=bound).astype(held_as)


def setup_inputs(seed: int = 0) -> dict:
    splits = jax.random.split(jax.random.key(seed), 14)
    return {
        "features": normal_values(splits[0], (LENGTH, CHANNELS), 1.0, 6.0, ((0, 256), (1, 2))),
        "lambda_real": draw_lambda_real(jax.random.fold_in(splits[13], 71), 0),
        "lambda_imag": jnp.clip(0.5 + 200.56177 * jax.random.uniform(splits[2], (GROUPS, STATE), jnp.float32) ** block_levels(splits[2], (GROUPS, STATE), ((0, 2),), -0.2, 0.2), 0.5, 201.06177),
        "log_step": draw_log_step(jax.random.fold_in(splits[13], 71), 0),
        "input_real": normal_values(splits[4], (GROUPS, STATE, GROUP), (max(4, LENGTH // 512)) ** -0.5, 0.5, ((0, 2),), jnp.float32),
        "input_imag": normal_values(splits[5], (GROUPS, STATE, GROUP), (max(4, LENGTH // 512)) ** -0.5, 0.5, ((0, 2),), jnp.float32),
        "real_output": normal_values(splits[6], (GROUPS, GROUP, STATE), STATE ** -0.5, 0.75, ((0, 2),), jnp.float32),
        "imaginary_output": normal_values(splits[7], (GROUPS, GROUP, STATE), STATE ** -0.5, 0.75, ((0, 2),), jnp.float32),
        "skip_gain": normal_values(splits[8], (CHANNELS,), 1.0, 4.0, ((0, 2),), jnp.float32),
        "value_weight": normal_values(splits[9], (CHANNELS, D), CHANNELS ** -0.5, 0.1875, ((0, 2),)),
        "gate_weight": normal_values(splits[10], (CHANNELS, D), CHANNELS ** -0.5, 0.1875, ((0, 2),)),
        "value_bias": normal_values(splits[11], (D,), 0.5, 3.0, (), jnp.float32),
        "gate_bias": normal_values(splits[12], (D,), 0.5, 3.0, (), jnp.float32),
    }


def discretize(lambda_real, lambda_imag, log_step, input_real, input_imag):
    step_size = jnp.exp(log_step)[:, None]
    magnitude = jnp.exp(lambda_real * step_size)
    phase_arg = lambda_imag * step_size
    trans_re = magnitude * jnp.cos(phase_arg)
    trans_im = magnitude * jnp.sin(phase_arg)
    denominator = lambda_real * lambda_real + lambda_imag * lambda_imag
    num_re = trans_re - 1.0
    num_im = trans_im
    f_re = (num_re * lambda_real + num_im * lambda_imag) / denominator
    f_im = (num_im * lambda_real - num_re * lambda_imag) / denominator
    bar_re = f_re[..., None] * input_real - f_im[..., None] * input_imag
    bar_im = f_re[..., None] * input_imag + f_im[..., None] * input_real
    return step_size, bar_re, bar_im


def powers(lambda_real, lambda_imag, step_size, positions):
    exponent = (jnp.arange(positions, dtype=jnp.int32) + 1).astype(jnp.float32)[:, None, None]
    magnitude = jnp.exp(exponent * lambda_real * step_size)
    phase_arg = exponent * lambda_imag * step_size
    return magnitude * jnp.cos(phase_arg), magnitude * jnp.sin(phase_arg)


def combine(earlier, later):
    a1r, a1i, b1r, b1i = earlier
    a2r, a2i, b2r, b2i = later
    return (a1r * a2r - a1i * a2i, a1r * a2i + a1i * a2r,
            a2r * b1r - a2i * b1i + b2r, a2r * b1i + a2i * b1r + b2i)


def local_states(trans_re, trans_im, bu_re, bu_im):
    a_re = jnp.broadcast_to(trans_re, bu_re.shape)
    a_im = jnp.broadcast_to(trans_im, bu_im.shape)
    result = lax.associative_scan(combine, (a_re, a_im, bu_re, bu_im), axis=0)
    return result[2], result[3]


def reference(features, lambda_real, lambda_imag, log_step, input_real, input_imag, real_output,
              imaginary_output, skip_gain, value_weight, gate_weight, value_bias, gate_bias):
    upper_limit = lax.Precision.HIGHEST
    step_size, bar_re, bar_im = discretize(lambda_real, lambda_imag, log_step, input_real, input_imag)
    pw_re, pw_im = powers(lambda_real, lambda_imag, step_size, TOK_SP)
    blocks = features.reshape(LENGTH // TOK_SP, TOK_SP, CHANNELS)
    slice_width = CHANNELS // N_TP

    def partials(activated, weight):
        total = jnp.zeros((TOK_SP, D), jnp.float32)
        for index in range(N_TP):
            left = activated[:, index * slice_width:(index + 1) * slice_width]
            right = weight[index * slice_width:(index + 1) * slice_width]
            rounded = lax.optimization_barrier(jnp.dot(left, right, preferred_element_type=jnp.float32).astype(jnp.bfloat16))
            total = total + rounded.astype(jnp.float32)
        return total

    def advance(carried, rows_per_block):
        h_re, h_im = carried
        widened = rows_per_block.astype(jnp.float32)
        grouped = widened.reshape(TOK_SP, GROUPS, GROUP)
        bu_re = jnp.einsum('sgc,gpc->sgp', grouped, bar_re, precision=upper_limit)
        bu_im = jnp.einsum('sgc,gpc->sgp', grouped, bar_im, precision=upper_limit)
        signal_real, signal_imaginary = local_states(pw_re[0], pw_im[0], bu_re, bu_im)
        signal_real = signal_real + pw_re * h_re - pw_im * h_im
        signal_imaginary = signal_imaginary + pw_re * h_im + pw_im * h_re
        mixer_response = (jnp.einsum('qej,eoj->qeo', signal_real, real_output, precision=upper_limit)
                    - jnp.einsum('qej,eoj->qeo', signal_imaginary, imaginary_output, precision=upper_limit))
        mixer_response = mixer_response.reshape(TOK_SP, CHANNELS) + skip_gain * widened
        activated = jax.nn.gelu(mixer_response).astype(jnp.bfloat16)
        value_sum = partials(activated, value_weight) + value_bias
        gate_sum = partials(activated, gate_weight) + gate_bias
        result = (value_sum * jax.nn.sigmoid(gate_sum)).astype(jnp.bfloat16)
        return (signal_real[-1], signal_imaginary[-1]), result

    start_state = (jnp.zeros((GROUPS, STATE), jnp.float32), jnp.zeros((GROUPS, STATE), jnp.float32))
    _, outputs = lax.scan(advance, start_state, blocks)
    return outputs.reshape(LENGTH, D)
```

```python
import functools

import jax
import jax.numpy as jnp
from jax import lax
from jax.experimental import pallas as pl
from jax.experimental.pallas import tpu as pltpu
from jax.sharding import Mesh
from jax.sharding import PartitionSpec as P

SP = ("z", "y", "x")
SP_TP = ("z", "y", "x", "tp")
NEAR = ("y", "x")
FAR = "z"

T = 256
BLOCKS = 8
STEPS = 32
G = 32
STATE = 64
GROUP = 16
CH = 512
FLAT = 2048
LB = 16
HALF = 1024
Q = 4

F32 = jnp.float32
BF16 = jnp.bfloat16
VMEM = pltpu.VMEM


def cmul(ar, ai, br, bi):
    return ar * br - ai * bi, ar * bi + ai * br


def power_rows(a_ref, lo, n):
    return jnp.concatenate(
        [jnp.broadcast_to(a_ref[pl.ds(lo + k, 1), :], (BLOCKS, 128)) for k in range(n)], axis=1
    )


def transition(lr_ref, li_ref, ls_ref):
    row = lax.broadcasted_iota(jnp.int32, (G, STATE), 0)
    logs = jnp.zeros((G, STATE), F32)
    for g in range(G):
        logs = jnp.where(row == g, ls_ref[g], logs)
    step = jnp.exp(logs)
    lr = lr_ref[...]
    li = li_ref[...]
    magnitude = jnp.exp(lr * step)
    phase = li * step
    return lr, li, magnitude * jnp.cos(phase), magnitude * jnp.sin(phase)


def order_matrix(transposed):
    r = lax.broadcasted_iota(jnp.int32, (T, T), 1 if transposed else 0)
    t = lax.broadcasted_iota(jnp.int32, (T, T), 0 if transposed else 1)
    hit = t == (r & 7) * STEPS + (r >> 3)
    return jnp.where(hit, 1.0, 0.0).astype(BF16)


def fold_groups(a):
    row = lax.broadcasted_iota(jnp.int32, (LB, G), 0)
    col = lax.broadcasted_iota(jnp.int32, (LB, G), 1)
    even = jnp.where(col == 2 * row, 1.0, 0.0)
    odd = jnp.where(col == 2 * row + 1, 1.0, 0.0)
    hi = lax.Precision.HIGHEST
    left = jnp.dot(even, a, precision=hi, preferred_element_type=F32)
    right = jnp.dot(odd, a, precision=hi, preferred_element_type=F32)
    return jnp.concatenate([left, right], axis=1)


def first_kernel(
    u_ref, lr_ref, li_ref, ls_ref, br_ref, bi_ref,
    copies_ref, whole_ref, ent_ref, up_ref, xr_ref, xi_ref, a_ref, f_ref,
    fin_ref, pw_ref,
):
    lr, li, ar, ai = transition(lr_ref, li_ref, ls_ref)
    den = lr * lr + li * li
    num = ar - 1.0
    f_ref[0] = (num * lr + ai * li) / den
    f_ref[1] = (ai * lr - num * li) / den

    pr, pi = fold_groups(ar), fold_groups(ai)
    a_ref[0], a_ref[1] = pr, pi
    for _ in range(5):
        pr, pi = cmul(pr, pi, pr, pi)
    for k in range(3):
        pw_ref[2 * k], pw_ref[2 * k + 1] = pr, pi
        a_ref[2 + 2 * k], a_ref[3 + 2 * k] = pr, pi
        pr, pi = cmul(pr, pi, pr, pi)
    whole_ref[0], whole_ref[1] = pr, pi

    up = jnp.dot(order_matrix(False), u_ref[...], preferred_element_type=F32).astype(BF16)
    up_ref[...] = up

    c = lax.broadcasted_iota(jnp.int32, (GROUP, 128), 0)
    lane = lax.broadcasted_iota(jnp.int32, (GROUP, 128), 1)
    spread = jnp.where((lane & 15) == c, 1.0, 0.0).astype(BF16)
    own = (lax.broadcasted_iota(jnp.int32, (512, 128), 0) >> 6) == (
        lax.broadcasted_iota(jnp.int32, (512, 128), 1) >> 4
    )
    for q in range(Q):
        for b_ref, x_ref in ((br_ref, xr_ref), (bi_ref, xi_ref)):
            b = b_ref[pl.ds(512 * q, 512), :].astype(BF16)
            wide = jnp.dot(b, spread, preferred_element_type=F32)
            wide = jnp.where(own, wide, 0.0).astype(BF16)
            x_ref[:, pl.ds(512 * q, 512)] = lax.dot_general(
                up[:, 128 * q : 128 * (q + 1)], wide, (((1,), (1,)), ((), ())),
                preferred_element_type=F32,
            )

    sub = lax.broadcasted_iota(jnp.int32, (BLOCKS, HALF), 0)
    for h in range(2):
        mr = power_rows(a_ref.at[0], 8 * h, 8)
        mi = power_rows(a_ref.at[1], 8 * h, 8)

        def body(j, carried):
            hr, hi = carried
            rows = pl.ds(pl.multiple_of(j * BLOCKS, BLOCKS), BLOCKS)
            nr, ni = cmul(mr, mi, hr, hi)
            nr = nr + xr_ref[rows, pl.ds(HALF * h, HALF)]
            ni = ni + xi_ref[rows, pl.ds(HALF * h, HALF)]
            return nr, ni

        zero = jnp.zeros((BLOCKS, HALF), F32)
        er, ei = lax.fori_loop(0, STEPS, body, (zero, zero), unroll=4)
        for k in range(3):
            s = 1 << k
            qr = power_rows(pw_ref.at[2 * k], 8 * h, 8)
            qi = power_rows(pw_ref.at[2 * k + 1], 8 * h, 8)
            shr = jnp.where(sub >= s, pltpu.roll(er, s, 0), 0.0)
            shi = jnp.where(sub >= s, pltpu.roll(ei, s, 0), 0.0)
            dr, di = cmul(qr, qi, shr, shi)
            er, ei = er + dr, ei + di
        for k in range(8):
            fin_ref[pl.ds(8 * h + k, 1), :] = er[7:8, 128 * k : 128 * (k + 1)]
            fin_ref[pl.ds(16 + 8 * h + k, 1), :] = ei[7:8, 128 * k : 128 * (k + 1)]
        ent_ref[0, :, pl.ds(HALF * h, HALF)] = jnp.where(sub >= 1, pltpu.roll(er, 1, 0), 0.0)
        ent_ref[1, :, pl.ds(HALF * h, HALF)] = jnp.where(sub >= 1, pltpu.roll(ei, 1, 0), 0.0)

    fin = fin_ref[...].astype(BF16)
    for m in range(copies_ref.shape[0]):
        copies_ref[m] = fin


def horner(n, index, parts, wr, wi):
    tr, ti = jnp.zeros((LB, 128), F32), jnp.zeros((LB, 128), F32)
    br, bi = tr, ti
    pr, pi = tr + 1.0, ti
    ir, ii = pr, pi
    for k in range(n):
        here = index == k
        br, bi = jnp.where(here, tr, br), jnp.where(here, ti, bi)
        ir, ii = jnp.where(here, pr, ir), jnp.where(here, pi, ii)
        part = parts[k].astype(F32)
        mr, mi = cmul(wr, wi, tr, ti)
        tr, ti = mr + part[:LB], mi + part[LB:]
        pr, pi = cmul(wr, wi, pr, pi)
    return tr, ti, br, bi, ir, ii, pr, pi


def near_kernel(index_ref, parts_ref, whole_ref, copies_ref, near_ref):
    n = parts_ref.shape[0]
    tr, ti, br, bi, ir, ii, pr, pi = horner(
        n, index_ref[0], parts_ref, whole_ref[0], whole_ref[1]
    )
    for k, value in enumerate((br, bi, ir, ii, pr, pi)):
        near_ref[k] = value
    total = jnp.concatenate([tr, ti], axis=0).astype(BF16)
    for m in range(copies_ref.shape[0]):
        copies_ref[m] = total


def gelu(x):
    return 0.5 * x * (1.0 + jnp.tanh(0.7978845608028654 * (x + 0.044715 * (x * x * x))))


def second_kernel(
    index_ref, parts_ref, near_ref, ent_ref, up_ref, xr_ref, xi_ref, a_ref, f_ref,
    cr_ref, ci_ref, skip_ref, vw_hbm, gw_hbm,
    give_ref, keep_ref,
    sr_ref, si_ref, in_ref, dr_ref, di_ref, act_ref, vw_ref, gw_ref, sem,
):
    vcopy = pltpu.make_async_copy(vw_hbm, vw_ref, sem.at[0])
    gcopy = pltpu.make_async_copy(gw_hbm, gw_ref, sem.at[1])
    vcopy.start()
    gcopy.start()

    n = parts_ref.shape[0]
    _, _, gr, gi, _, _, _, _ = horner(n, index_ref[0], parts_ref, near_ref[4], near_ref[5])
    er, ei = cmul(near_ref[2], near_ref[3], gr, gi)
    in_ref[0], in_ref[1] = near_ref[0] + er, near_ref[1] + ei

    for g in range(G):
        rows = pl.ds(GROUP * g, GROUP)
        fr, fi = f_ref[0, pl.ds(g, 1), :], f_ref[1, pl.ds(g, 1), :]
        cr, ci = cr_ref[rows, :], ci_ref[rows, :]
        dr_ref[rows, :] = cr * fr - ci * fi
        di_ref[rows, :] = -(cr * fi + ci * fr)

    sub = lax.broadcasted_iota(jnp.int32, (BLOCKS, HALF), 0)
    for h in range(2):
        cols = pl.ds(HALF * h, HALF)
        mr, mi = power_rows(in_ref.at[0], 8 * h, 8), power_rows(in_ref.at[1], 8 * h, 8)
        for k in range(3):
            bit = (sub & (1 << k)) != 0
            qr = jnp.where(bit, power_rows(a_ref.at[2 + 2 * k], 8 * h, 8), 1.0)
            qi = jnp.where(bit, power_rows(a_ref.at[3 + 2 * k], 8 * h, 8), 0.0)
            mr, mi = cmul(qr, qi, mr, mi)
        er, ei = ent_ref[0, :, cols] + mr, ent_ref[1, :, cols] + mi
        mr, mi = power_rows(a_ref.at[0], 8 * h, 8), power_rows(a_ref.at[1], 8 * h, 8)

        def body(j, carried):
            hr, hi = carried
            rs, ims = [], []
            for step in range(2):
                rows = pl.ds(pl.multiple_of(j * 16, 16) + 8 * step, BLOCKS)
                nr, ni = cmul(mr, mi, hr, hi)
                hr = nr + xr_ref[rows, cols]
                hi = ni + xi_ref[rows, cols]
                rs.append(hr)
                ims.append(hi)
            rows = pl.ds(pl.multiple_of(j * 16, 16), 16)
            sr_ref[rows, cols] = jnp.concatenate(rs, axis=0).astype(BF16)
            si_ref[rows, cols] = jnp.concatenate(ims, axis=0).astype(BF16)
            return hr, hi

        lax.fori_loop(0, STEPS // 2, body, (er, ei), unroll=2)

    own = (lax.broadcasted_iota(jnp.int32, (128, 512), 0) >> 4) == (
        lax.broadcasted_iota(jnp.int32, (128, 512), 1) >> 6
    )
    for q in range(Q):
        total = skip_ref[:, pl.ds(128 * q, 128)] * up_ref[:, pl.ds(128 * q, 128)].astype(F32)
        for d_ref, s_ref in ((dr_ref, sr_ref), (di_ref, si_ref)):
            d = d_ref[pl.ds(128 * q, 128), :]
            wide = jnp.where(own, jnp.concatenate([d] * 8, axis=1), 0.0).astype(BF16)
            total = total + lax.dot_general(
                s_ref[:, pl.ds(512 * q, 512)], wide, (((1,), (1,)), ((), ())),
                preferred_element_type=F32,
            )
        act_ref[:, pl.ds(128 * q, 128)] = gelu(total).astype(BF16)

    act_ref[...] = jnp.dot(
        order_matrix(True), act_ref[...], preferred_element_type=F32
    ).astype(BF16)
    half = T // 2
    tp = index_ref[1]
    mine = act_ref[pl.ds(pl.multiple_of(tp * half, half), half), :]
    theirs = act_ref[pl.ds(pl.multiple_of((1 - tp) * half, half), half), :]
    width = vw_ref.shape[1]
    for copy, w_ref, k in ((vcopy, vw_ref, 0), (gcopy, gw_ref, 1)):
        copy.wait()
        for rows, out_ref in ((theirs, give_ref), (mine, keep_ref)):
            out_ref[:, pl.ds(width * k, width)] = jnp.dot(
                rows, w_ref[...], preferred_element_type=F32
            ).astype(BF16)


def call(kernel, outs, ins, scratch=(), name=None):
    return pl.pallas_call(
        kernel,
        out_shape=[jax.ShapeDtypeStruct(s, d) for s, d in outs],
        in_specs=[pl.BlockSpec(memory_space=m) for m in ins],
        out_specs=[pl.BlockSpec(memory_space=VMEM)] * len(outs),
        scratch_shapes=list(scratch),
        compiler_params=pltpu.CompilerParams(vmem_limit_bytes=56 * 1024 * 1024),
        name=name,
    )


def to_all(copies, axes):
    return lax.all_to_all(copies, axes, split_axis=0, concat_axis=0, tiled=True)


def local(
    features, lambda_real, lambda_imag, log_step, input_real, input_imag, real_output,
    imaginary_output, skip_gain, value_weight, gate_weight, value_bias, gate_bias,
):
    n_near = lax.axis_size("y") * lax.axis_size("x")
    n_far = lax.axis_size(FAR)
    near_index = lax.axis_index("y") * lax.axis_size("x") + lax.axis_index("x")
    far_index = lax.axis_index(FAR)
    tp = lax.axis_index("tp")
    near_at = jnp.stack([near_index]).astype(jnp.int32)
    far_at = jnp.stack([far_index, tp]).astype(jnp.int32)
    smem = pltpu.SMEM

    copies, whole, entering, up, xr, xi, powers, f = call(
        first_kernel,
        [
            ((n_near, 32, 128), BF16), ((2, LB, 128), F32), ((2, BLOCKS, FLAT), F32), ((T, CH), BF16),
            ((T, FLAT), F32), ((T, FLAT), F32), ((8, LB, 128), F32), ((2, G, STATE), F32),
        ],
        [VMEM, VMEM, VMEM, smem, VMEM, VMEM],
        [pltpu.VMEM((32, 128), F32), pltpu.VMEM((6, LB, 128), F32)],
        "first",
    )(
        features, lambda_real, lambda_imag, log_step,
        input_real.reshape(FLAT, GROUP), input_imag.reshape(FLAT, GROUP),
    )
    parts = to_all(copies, NEAR)
    totals, near = call(
        near_kernel,
        [((n_far, 32, 128), BF16), ((6, LB, 128), F32)],
        [smem, VMEM, VMEM],
        name="near",
    )(near_at, parts, whole)
    planes = to_all(totals, FAR)
    width = value_weight.shape[1]
    give, keep = call(
        second_kernel,
        [((T // 2, 2 * width), BF16), ((T // 2, 2 * width), BF16)],
        [smem] + [VMEM] * 11 + [pl.ANY] * 2,
        [
            pltpu.VMEM((T, FLAT), BF16), pltpu.VMEM((T, FLAT), BF16), pltpu.VMEM((2, LB, 128), F32),
            pltpu.VMEM((CH, STATE), F32), pltpu.VMEM((CH, STATE), F32), pltpu.VMEM((T, CH), BF16),
            pltpu.VMEM((CH, width), BF16), pltpu.VMEM((CH, width), BF16), pltpu.SemaphoreType.DMA((2,)),
        ],
        "second",
    )(
        far_at, planes, near, entering, up, xr, xi, powers, f,
        real_output.reshape(CH, STATE), imaginary_output.reshape(CH, STATE),
        skip_gain.reshape(1, CH), value_weight, gate_weight,
    )
    got = lax.ppermute(give, "tp", [(0, 1), (1, 0)])
    total = keep.astype(F32) + got.astype(F32)
    value_sum = total[:, :width] + value_bias
    gate_sum = total[:, width:] + gate_bias
    return (value_sum * jax.nn.sigmoid(gate_sum)).astype(BF16)


def solution(mesh):
    split = Mesh(mesh.devices.reshape(8, 8, 4, mesh.shape["tp"]), SP_TP)
    in_specs = (
        P(SP, "tp"),
        P("tp", None),
        P("tp", None),
        P("tp"),
        P("tp", None, None),
        P("tp", None, None),
        P("tp", None, None),
        P("tp", None, None),
        P("tp"),
        P("tp", None),
        P("tp", None),
        P(),
        P(),
    )
    return jax.shard_map(local, mesh=split, in_specs=in_specs, out_specs=P(SP_TP, None), check_vma=False)
```

```python
import jax
import jax.numpy as jnp
from jax import lax
from jax.experimental import pallas as pl
from jax.experimental.pallas import tpu as pltpu
from jax.sharding import Mesh
from jax.sharding import PartitionSpec as P

SP = ("z", "y", "x")
SP_TP = ("z", "y", "x", "tp")
NEAR = ("y", "x")
FAR = ("z", "tp")
SWAP = [(0, 1), (1, 0)]

T = 256
BLOCKS = 8
STEPS = 32
G = 32
STATE = 64
GROUP = 16
CH = 512
FLAT = 2048
LB = 16
HALF = 1024
Q = 4
HROWS = 128
HALF_D = CH // 2
PACK = 2 * CH + 4 * LB
CHUNK = 512

F32 = jnp.float32
BF16 = jnp.bfloat16
VMEM = pltpu.VMEM


def cmul(ar, ai, br, bi):
    return ar * br - ai * bi, ar * bi + ai * br


def power_rows(a_ref, lo, n):
    return jnp.concatenate(
        [jnp.broadcast_to(a_ref[pl.ds(lo + k, 1), :], (BLOCKS, 128)) for k in range(n)], axis=1
    )


def transition(lr_ref, li_ref, ls_ref):
    row = lax.broadcasted_iota(jnp.int32, (G, STATE), 0)
    logs = jnp.zeros((G, STATE), F32)
    for g in range(G):
        logs = jnp.where(row == g, ls_ref[g], logs)
    step = jnp.exp(logs)
    lr = lr_ref[...]
    li = li_ref[...]
    magnitude = jnp.exp(lr * step)
    phase = li * step
    return lr, li, magnitude * jnp.cos(phase), magnitude * jnp.sin(phase)


def order_matrix(transposed):
    r = lax.broadcasted_iota(jnp.int32, (T, T), 1 if transposed else 0)
    t = lax.broadcasted_iota(jnp.int32, (T, T), 0 if transposed else 1)
    hit = t == (r & 7) * STEPS + (r >> 3)
    return jnp.where(hit, 1.0, 0.0).astype(BF16)


def fold_groups(a):
    row = lax.broadcasted_iota(jnp.int32, (LB, G), 0)
    col = lax.broadcasted_iota(jnp.int32, (LB, G), 1)
    even = jnp.where(col == 2 * row, 1.0, 0.0)
    odd = jnp.where(col == 2 * row + 1, 1.0, 0.0)
    hi = lax.Precision.HIGHEST
    left = jnp.dot(even, a, precision=hi, preferred_element_type=F32)
    right = jnp.dot(odd, a, precision=hi, preferred_element_type=F32)
    return jnp.concatenate([left, right], axis=1)


def put_inputs(u, br_ref, bi_ref, xr_ref, xi_ref):
    up = jnp.dot(order_matrix(False), u, preferred_element_type=F32).astype(BF16)
    own = (lax.broadcasted_iota(jnp.int32, (128, 512), 0) >> 4) == (
        lax.broadcasted_iota(jnp.int32, (128, 512), 1) >> 6
    )
    for q in range(Q):
        for b_ref, x_ref in ((br_ref, xr_ref), (bi_ref, xi_ref)):
            b = b_ref[pl.ds(128 * q, 128), :]
            wide = jnp.where(own, jnp.concatenate([b] * 8, axis=1), 0.0).astype(BF16)
            x_ref[:, pl.ds(512 * q, 512)] = jnp.dot(
                up[:, 128 * q : 128 * (q + 1)], wide, preferred_element_type=F32
            )
    return up


def fetch(sources, targets, sem):
    moves = [
        pltpu.make_async_copy(src, dst, sem.at[k])
        for k, (src, dst) in enumerate(zip(sources, targets, strict=True))
    ]
    for move in moves:
        move.start()
    return moves


def first_kernel(
    ls_hbm, lr_hbm, li_hbm, u_hbm, br_hbm, bi_hbm,
    copies_ref, a_ref, ent_ref,
    xr_ref, xi_ref, fin_ref, pw_ref, ls_ref, lr_ref, li_ref, u_ref, br_ref, bi_ref, sem,
):
    moves = fetch(
        (ls_hbm, lr_hbm, li_hbm, u_hbm, br_hbm, bi_hbm),
        (ls_ref, lr_ref, li_ref, u_ref, br_ref, bi_ref), sem,
    )
    for move in moves[:3]:
        move.wait()
    _, _, ar, ai = transition(lr_ref, li_ref, ls_ref)
    pr, pi = fold_groups(ar), fold_groups(ai)
    a_ref[0], a_ref[1] = pr, pi
    for _ in range(5):
        pr, pi = cmul(pr, pi, pr, pi)
    for k in range(3):
        pw_ref[2 * k], pw_ref[2 * k + 1] = pr, pi
        pr, pi = cmul(pr, pi, pr, pi)
    a_ref[2], a_ref[3] = pr, pi
    for move in moves[3:]:
        move.wait()
    put_inputs(u_ref[...], br_ref, bi_ref, xr_ref, xi_ref)

    sub = lax.broadcasted_iota(jnp.int32, (BLOCKS, HALF), 0)
    for h in range(2):
        mr = power_rows(a_ref.at[0], 8 * h, 8)
        mi = power_rows(a_ref.at[1], 8 * h, 8)

        def body(j, carried):
            hr, hi = carried
            rows = pl.ds(pl.multiple_of(j * BLOCKS, BLOCKS), BLOCKS)
            nr, ni = cmul(mr, mi, hr, hi)
            nr = nr + xr_ref[rows, pl.ds(HALF * h, HALF)]
            ni = ni + xi_ref[rows, pl.ds(HALF * h, HALF)]
            return nr, ni

        zero = jnp.zeros((BLOCKS, HALF), F32)
        er, ei = lax.fori_loop(0, STEPS, body, (zero, zero), unroll=4)
        for k in range(3):
            s = 1 << k
            qr = power_rows(pw_ref.at[2 * k], 8 * h, 8)
            qi = power_rows(pw_ref.at[2 * k + 1], 8 * h, 8)
            shr = jnp.where(sub >= s, pltpu.roll(er, s, 0), 0.0)
            shi = jnp.where(sub >= s, pltpu.roll(ei, s, 0), 0.0)
            dr, di = cmul(qr, qi, shr, shi)
            er, ei = er + dr, ei + di
        for k in range(8):
            fin_ref[pl.ds(8 * h + k, 1), :] = er[7:8, 128 * k : 128 * (k + 1)]
            fin_ref[pl.ds(16 + 8 * h + k, 1), :] = ei[7:8, 128 * k : 128 * (k + 1)]
        ent_ref[0, :, pl.ds(HALF * h, HALF)] = jnp.where(sub >= 1, pltpu.roll(er, 1, 0), 0.0)
        ent_ref[1, :, pl.ds(HALF * h, HALF)] = jnp.where(sub >= 1, pltpu.roll(ei, 1, 0), 0.0)

    fin = fin_ref[...].astype(BF16)
    for m in range(copies_ref.shape[0]):
        copies_ref[m] = fin


def spread_pairs(parts):
    left = lax.broadcasted_iota(jnp.int32, (GROUP, 128), 1) < STATE
    zero = jnp.zeros((32, 128), BF16)
    rows = []
    for k, part in enumerate(parts):
        block = jnp.concatenate([jnp.where(left, part, 0.0), jnp.where(left, 0.0, part)], axis=0)
        rows.append(jnp.concatenate([block.astype(BF16) if j == k else zero for j in range(4)], axis=1))
    return jnp.concatenate(rows, axis=0)


def local_kernel(
    index_ref, ls_hbm, lr_hbm, li_hbm, cr_hbm, ci_hbm, u_hbm, br_hbm, bi_hbm, skip_hbm, a_ref, ent_ref,
    keep_ref, mine_ref, pack_ref,
    xr_ref, xi_ref, sr_ref, si_ref, y_ref,
    ls_ref, lr_ref, li_ref, cr_ref, ci_ref, u_ref, br_ref, bi_ref, skip_ref, sem,
):
    for move in fetch(
        (ls_hbm, lr_hbm, li_hbm, cr_hbm, ci_hbm, u_hbm, br_hbm, bi_hbm, skip_hbm),
        (ls_ref, lr_ref, li_ref, cr_ref, ci_ref, u_ref, br_ref, bi_ref, skip_ref), sem,
    ):
        move.wait()
    lr, li, ar, ai = transition(lr_ref, li_ref, ls_ref)
    den = lr * lr + li * li
    num = ar - 1.0
    fr = (num * lr + ai * li) / den
    fi = (ai * lr - num * li) / den
    for k in range(LB):
        pairs = []
        for g in (2 * k, 2 * k + 1):
            rows = pl.ds(GROUP * g, GROUP)
            pairs.append(cmul(cr_ref[rows, :], ci_ref[rows, :], fr[g : g + 1, :], fi[g : g + 1, :]))
        for c in range(2):
            d = jnp.concatenate([pairs[0][c], pairs[1][c]], axis=1)
            rows = pl.ds(HALF_D * c + GROUP * k, GROUP)
            mine_ref[rows, :] = d
            pack_ref[rows, :] = d
    for k in range(4):
        pack_ref[pl.ds(2 * CH + LB * k, LB), :] = a_ref[k]

    up = put_inputs(u_ref[...], br_ref, bi_ref, xr_ref, xi_ref)
    for h in range(2):
        cols = pl.ds(HALF * h, HALF)
        mr, mi = power_rows(a_ref.at[0], 8 * h, 8), power_rows(a_ref.at[1], 8 * h, 8)

        def body(j, carried):
            hr, hi = carried
            rs, ims = [], []
            for step in range(2):
                rows = pl.ds(pl.multiple_of(j * 16, 16) + 8 * step, BLOCKS)
                nr, ni = cmul(mr, mi, hr, hi)
                hr = nr + xr_ref[rows, cols]
                hi = ni + xi_ref[rows, cols]
                rs.append(hr)
                ims.append(hi)
            rows = pl.ds(pl.multiple_of(j * 16, 16), 16)
            sr_ref[rows, cols] = jnp.concatenate(rs, axis=0).astype(BF16)
            si_ref[rows, cols] = jnp.concatenate(ims, axis=0).astype(BF16)
            return hr, hi

        lax.fori_loop(0, STEPS // 2, body, (ent_ref[0, :, cols], ent_ref[1, :, cols]), unroll=2)

    for q in range(Q):
        cols = pl.ds(128 * q, 128)
        total = skip_ref[:, cols] * up[:, 128 * q : 128 * (q + 1)].astype(F32)
        for c, s_ref in enumerate((sr_ref, si_ref)):
            d = [mine_ref[pl.ds(HALF_D * c + GROUP * (4 * q + k), GROUP), :] for k in range(4)]
            wide = spread_pairs(d if c == 0 else [-part for part in d])
            total = total + lax.dot_general(
                s_ref[:, pl.ds(512 * q, 512)], wide, (((1,), (1,)), ((), ())),
                preferred_element_type=F32,
            )
        y_ref[:, cols] = total
    y_ref[...] = jnp.dot(
        order_matrix(True).astype(F32), y_ref[...],
        precision=lax.Precision.HIGHEST, preferred_element_type=F32,
    )
    tp = index_ref[2]
    mine = pl.ds(pl.multiple_of(tp * HROWS, HROWS), HROWS)
    theirs = pl.ds(pl.multiple_of((1 - tp) * HROWS, HROWS), HROWS)
    keep_ref[...] = y_ref[mine, :]
    for q in range(Q):
        pack_ref[pl.ds(CH + HROWS * q, HROWS), :] = y_ref[theirs, pl.ds(128 * q, 128)]


def near_kernel(index_ref, parts_ref, a_ref, copies_ref):
    wr, wi = a_ref[2], a_ref[3]
    index = index_ref[0]
    tr, ti = jnp.zeros((LB, 128), F32), jnp.zeros((LB, 128), F32)
    br, bi = tr, ti
    for k in range(parts_ref.shape[0]):
        here = index == k
        br, bi = jnp.where(here, tr, br), jnp.where(here, ti, bi)
        part = parts_ref[k].astype(F32)
        mr, mi = cmul(wr, wi, tr, ti)
        tr, ti = mr + part[:LB], mi + part[LB:]
    total = jnp.concatenate([tr, ti], axis=0).astype(BF16)
    before = jnp.concatenate([br, bi], axis=0).astype(BF16)
    for m in range(copies_ref.shape[0]):
        copies_ref[m] = jnp.where(index_ref[1] == m // 2, before, total)


def prepare_kernel(
    index_ref, mine_ref, other_ref,
    tr_ref, ti_ref, pw_ref,
    a_ref,
):
    near, tp = index_ref[0], index_ref[2]
    sub = lax.broadcasted_iota(jnp.int32, (BLOCKS, HALF), 0)
    for o in range(2):
        pack_ref, at = (mine_ref, 0) if o == 0 else (other_ref, 2 * CH)
        pr, pi, wr, wi = (
            pack_ref[k] if o == 0 else pack_ref[pl.ds(at + LB * k, LB), :] for k in range(4)
        )
        base = pr, pi
        pr, pi = wr, wi
        ir, ii = jnp.ones((LB, 128), F32), jnp.zeros((LB, 128), F32)
        for k in range(5):
            bit = ((near >> k) & 1) == 1
            jr, ji = cmul(ir, ii, pr, pi)
            ir, ii = jnp.where(bit, jr, ir), jnp.where(bit, ji, ii)
            pr, pi = cmul(pr, pi, pr, pi)
        pw_ref[o, 0], pw_ref[o, 1], pw_ref[o, 2], pw_ref[o, 3] = ir, ii, pr, pi

        pr, pi = base
        for k in range(8):
            a_ref[2 * k], a_ref[2 * k + 1] = pr, pi
            pr, pi = cmul(pr, pi, pr, pi)
        for h in range(2):
            cols = pl.ds(HALF * h, HALF)

            def power(k):
                return power_rows(a_ref.at[2 * k], 8 * h, 8), power_rows(a_ref.at[2 * k + 1], 8 * h, 8)

            mr, mi = power(0)
            for k, bit in ((0, (sub & 1) != 0), (1, (sub & 2) != 0), (2, (sub & 4) != 0), (7, tp == 1)):
                qr, qi = power(k)
                jr, ji = cmul(mr, mi, qr, qi)
                mr, mi = jnp.where(bit, jr, mr), jnp.where(bit, ji, mi)
            er, ei = power(3)

            def body(j, carried):
                hr, hi = carried
                nr, ni = cmul(er, ei, hr, hi)
                rows = pl.ds(pl.multiple_of(j * 16, 16), 16)
                tr_ref[o, rows, cols] = jnp.concatenate([hr, nr], axis=0).astype(BF16)
                ti_ref[o, rows, cols] = jnp.concatenate([hi, ni], axis=0).astype(BF16)
                return cmul(er, ei, nr, ni)

            lax.fori_loop(0, HROWS // 16, body, (mr, mi))


def gelu(x):
    return 0.5 * x * (1.0 + jnp.tanh(0.7978845608028654 * (x + 0.044715 * (x * x * x))))


def last_kernel(
    index_ref, parts_ref, keep_ref, mine_ref, other_ref, tr_ref, ti_ref, pw_ref,
    vw_hbm, gw_hbm, vo_hbm, go_hbm, vb_hbm, gb_hbm,
    out_ref,
    in_ref, act_ref, w_ref, vb_ref, gb_ref, sem,
):
    width = out_ref.shape[1]
    chunks = width // CHUNK
    moves = []
    for n in range(chunks):
        cols = pl.ds(CHUNK * n, CHUNK)
        for k, w_hbm in enumerate((vw_hbm, vo_hbm, gw_hbm, go_hbm)):
            moves.append(pltpu.make_async_copy(w_hbm.at[:, cols], w_ref.at[k, :, cols], sem.at[4 * n + k]))
    biases = [
        pltpu.make_async_copy(vb_hbm, vb_ref, sem.at[4 * chunks]),
        pltpu.make_async_copy(gb_hbm, gb_ref, sem.at[4 * chunks + 1]),
    ]
    for move in biases + moves:
        move.start()

    far, tp = index_ref[1], index_ref[2]
    n_far = parts_ref.shape[0] // 2
    for o in range(2):
        side = tp if o == 0 else 1 - tp
        wr, wi = pw_ref[o, 2], pw_ref[o, 3]
        gr, gi = jnp.zeros((LB, 128), F32), jnp.zeros((LB, 128), F32)
        for k in range(n_far - 1):
            part = parts_ref[2 * k + side].astype(F32)
            mr, mi = cmul(wr, wi, gr, gi)
            gr = jnp.where(k < far, mr + part[:LB], gr)
            gi = jnp.where(k < far, mi + part[LB:], gi)
        before = parts_ref[2 * far + side].astype(F32)
        mr, mi = cmul(pw_ref[o, 0], pw_ref[o, 1], gr, gi)
        in_ref[2 * o], in_ref[2 * o + 1] = before[:LB] + mr, before[LB:] + mi

    for o, d_ref in enumerate((mine_ref, other_ref)):
        for q in range(Q):
            real, imag = [], []
            for k in range(4 * q, 4 * q + 4):
                vr, vi = cmul(
                    d_ref[pl.ds(GROUP * k, GROUP), :], d_ref[pl.ds(HALF_D + GROUP * k, GROUP), :],
                    in_ref[2 * o, pl.ds(k, 1), :], in_ref[2 * o + 1, pl.ds(k, 1), :],
                )
                real.append(vr)
                imag.append(-vi)
            cols = pl.ds(128 * q, 128)
            total = keep_ref[:, cols] if o == 0 else other_ref[pl.ds(CH + HROWS * q, HROWS), :]
            for v, t_ref in ((real, tr_ref), (imag, ti_ref)):
                total = total + lax.dot_general(
                    t_ref[o, :, pl.ds(512 * q, 512)], spread_pairs(v), (((1,), (1,)), ((), ())),
                    preferred_element_type=F32,
                )
            act_ref[o, :, cols] = gelu(total).astype(BF16)

    def product(o, k, cols):
        return jnp.dot(act_ref[o], w_ref[k, :, cols], preferred_element_type=F32).astype(BF16).astype(F32)

    for move in biases:
        move.wait()
    for n in range(chunks):
        cols = pl.ds(CHUNK * n, CHUNK)
        for move in moves[4 * n : 4 * n + 4]:
            move.wait()
        value = product(0, 0, cols) + product(1, 1, cols) + vb_ref[:, cols]
        gate = product(0, 2, cols) + product(1, 3, cols) + gb_ref[:, cols]
        out_ref[:, cols] = (value * jax.nn.sigmoid(gate)).astype(BF16)


def call(kernel, outs, ins, scratch=(), limit=16):
    fn = pl.pallas_call(
        kernel,
        out_shape=[VMEM(s, d) if v else jax.ShapeDtypeStruct(s, d) for s, d, v in outs],
        in_specs=[pl.BlockSpec(memory_space=VMEM if m is True else m) for m in ins],
        out_specs=[pl.BlockSpec(memory_space=VMEM)] * len(outs),
        scratch_shapes=list(scratch),
        compiler_params=pltpu.CompilerParams(vmem_limit_bytes=limit * 1024 * 1024),
    )

    def run(*args):
        placed = []
        for a, m in zip(args, ins, strict=True):
            if m is True:
                a = pltpu.with_memory_space_constraint(a, VMEM)
            elif m is pltpu.HBM:
                a = pltpu.with_memory_space_constraint(a, pltpu.HBM)
            placed.append(a)
        return fn(*placed)

    return run


def to_all(copies, axes):
    return lax.all_to_all(copies, axes, split_axis=0, concat_axis=0, tiled=True)


def mixer(
    features, lambda_real, lambda_imag, log_step, input_real, input_imag, real_output,
    imaginary_output, skip_gain, value_weight, gate_weight, value_bias, gate_bias,
):
    n_near = lax.axis_size("y") * lax.axis_size("x")
    n_far = lax.axis_size("z")
    near_index = lax.axis_index("y") * lax.axis_size("x") + lax.axis_index("x")
    at = jnp.stack([near_index, lax.axis_index("z"), lax.axis_index("tp")]).astype(jnp.int32)
    smem, hbm = pltpu.SMEM, pltpu.HBM
    width = value_weight.shape[1]
    b_re = input_real.transpose(0, 2, 1).reshape(CH, STATE)
    b_im = input_imag.transpose(0, 2, 1).reshape(CH, STATE)
    params = (log_step, lambda_real, lambda_imag, b_re, b_im)
    rates = [smem((G,), F32), VMEM((G, STATE), F32), VMEM((G, STATE), F32)]
    matrix = [VMEM((CH, STATE), F32), VMEM((CH, STATE), F32)]

    copies, powers, entering = call(
        first_kernel,
        [((n_near, 32, 128), BF16, True), ((4, LB, 128), F32, True), ((2, BLOCKS, FLAT), F32, True)],
        [hbm] * 6,
        [
            VMEM((T, FLAT), F32), VMEM((T, FLAT), F32), VMEM((32, 128), F32), VMEM((6, LB, 128), F32),
            *rates, VMEM((T, CH), BF16), *matrix, pltpu.SemaphoreType.DMA((6,)),
        ],
        16,
    )(*params[:3], features, *params[3:])
    parts = to_all(copies, NEAR)
    keep, mine, pack = call(
        local_kernel,
        [((HROWS, CH), F32, True), ((CH, 128), F32, True), ((PACK, 128), F32, False)],
        [smem] + [hbm] * 9 + [True, True],
        [
            VMEM((T, FLAT), F32), VMEM((T, FLAT), F32), VMEM((T, FLAT), BF16), VMEM((T, FLAT), BF16),
            VMEM((T, CH), F32), *rates, *matrix, VMEM((T, CH), BF16), *matrix, VMEM((1, CH), F32),
            pltpu.SemaphoreType.DMA((9,)),
        ],
        20,
    )(
        at, *params[:3], real_output.reshape(CH, STATE), imaginary_output.reshape(CH, STATE),
        features, *params[3:], skip_gain.reshape(1, CH), powers, entering,
    )
    value_other = lax.ppermute(value_weight, "tp", SWAP)
    gate_other = lax.ppermute(gate_weight, "tp", SWAP)
    pack_other = lax.ppermute(pack, "tp", SWAP)
    (totals,) = call(near_kernel, [((2 * n_far, 32, 128), BF16, True)], [smem, True, True], limit=4)(at, parts, powers)
    planes = to_all(totals, FAR)
    prepared = call(
        prepare_kernel,
        [((2, HROWS, FLAT), BF16, True), ((2, HROWS, FLAT), BF16, True), ((2, 4, LB, 128), F32, True)],
        [smem, True, True],
        [VMEM((16, LB, 128), F32)],
    )(at, powers, pack_other)
    (out,) = call(
        last_kernel,
        [((HROWS, width), BF16, False)],
        [smem] + [True] * 7 + [hbm] * 6,
        [
            VMEM((4, LB, 128), F32), VMEM((2, HROWS, CH), BF16), VMEM((4, CH, width), BF16),
            VMEM((1, width), F32), VMEM((1, width), F32),
            pltpu.SemaphoreType.DMA((4 * (width // CHUNK) + 2,)),
        ],
        24,
    )(
        at, planes, keep, mine, pack_other, *prepared, value_weight, gate_weight, value_other, gate_other,
        value_bias.reshape(1, width), gate_bias.reshape(1, width),
    )
    return out


def solution(mesh):
    split = Mesh(mesh.devices.reshape(8, 8, 4, mesh.shape["tp"]), SP_TP)
    in_specs = (
        P(SP, "tp"),
        P("tp", None),
        P("tp", None),
        P("tp"),
        P("tp", None, None),
        P("tp", None, None),
        P("tp", None, None),
        P("tp", None, None),
        P("tp"),
        P("tp", None),
        P("tp", None),
        P(),
        P(),
    )
    return jax.shard_map(mixer, mesh=split, in_specs=in_specs, out_specs=P(SP_TP, None), check_vma=False)
```

```python
import jax
import jax.numpy as jnp
from jax import lax
from jax.experimental import pallas as pl
from jax.experimental.pallas import tpu as pltpu
from jax.sharding import Mesh
from jax.sharding import PartitionSpec as P

SP = ("z", "y", "x")
SP_TP = ("z", "y", "x", "tp")
NEAR = ("y", "x")
FAR = ("z", "tp")
SWAP = [(0, 1), (1, 0)]

T = 256
BLOCKS = 8
STEPS = 32
G = 32
STATE = 64
GROUP = 16
CH = 512
FLAT = 2048
LB = 16
HALF = 1024
Q = 4
HROWS = 128
HALF_D = CH // 2
PACK = 2 * CH + 4 * LB
CHUNK = 512

F32 = jnp.float32
BF16 = jnp.bfloat16
VMEM = pltpu.VMEM


def cmul(ar, ai, br, bi):
    return ar * br - ai * bi, ar * bi + ai * br


def power_rows(a_ref, lo, n):
    return jnp.concatenate(
        [jnp.broadcast_to(a_ref[pl.ds(lo + k, 1), :], (BLOCKS, 128)) for k in range(n)], axis=1
    )


def transition(lr_ref, li_ref, ls_ref):
    row = lax.broadcasted_iota(jnp.int32, (G, STATE), 0)
    logs = jnp.zeros((G, STATE), F32)
    for g in range(G):
        logs = jnp.where(row == g, ls_ref[g], logs)
    step = jnp.exp(logs)
    lr = lr_ref[...]
    li = li_ref[...]
    magnitude = jnp.exp(lr * step)
    phase = li * step
    return lr, li, magnitude * jnp.cos(phase), magnitude * jnp.sin(phase)


def order_matrix(transposed):
    r = lax.broadcasted_iota(jnp.int32, (T, T), 1 if transposed else 0)
    t = lax.broadcasted_iota(jnp.int32, (T, T), 0 if transposed else 1)
    hit = t == (r & 7) * STEPS + (r >> 3)
    return jnp.where(hit, 1.0, 0.0).astype(BF16)


def fold_groups(a):
    row = lax.broadcasted_iota(jnp.int32, (LB, G), 0)
    col = lax.broadcasted_iota(jnp.int32, (LB, G), 1)
    even = jnp.where(col == 2 * row, 1.0, 0.0)
    odd = jnp.where(col == 2 * row + 1, 1.0, 0.0)
    hi = lax.Precision.HIGHEST
    left = jnp.dot(even, a, precision=hi, preferred_element_type=F32)
    right = jnp.dot(odd, a, precision=hi, preferred_element_type=F32)
    return jnp.concatenate([left, right], axis=1)


def near_index():
    return lax.axis_index("y") * lax.axis_size("x") + lax.axis_index("x")


def put_inputs(u, br_ref, bi_ref, xr_ref, xi_ref):
    up = jnp.dot(order_matrix(False), u, preferred_element_type=F32).astype(BF16)
    own = (lax.broadcasted_iota(jnp.int32, (128, 512), 0) >> 4) == (
        lax.broadcasted_iota(jnp.int32, (128, 512), 1) >> 6
    )
    for q in range(Q):
        for b_ref, x_ref in ((br_ref, xr_ref), (bi_ref, xi_ref)):
            b = b_ref[pl.ds(128 * q, 128), :]
            wide = jnp.where(own, jnp.concatenate([b] * 8, axis=1), 0.0).astype(BF16)
            x_ref[:, pl.ds(512 * q, 512)] = jnp.dot(
                up[:, 128 * q : 128 * (q + 1)], wide, preferred_element_type=F32
            )
    return up


def fetch(sources, targets, sem):
    moves = [
        pltpu.make_async_copy(src, dst, sem.at[k])
        for k, (src, dst) in enumerate(zip(sources, targets, strict=True))
    ]
    for move in moves:
        move.start()
    return moves


def first_kernel(
    ls_hbm, lr_hbm, li_hbm, u_hbm, br_hbm, bi_hbm,
    copies_ref, a_ref, ent_ref,
    xr_ref, xi_ref, fin_ref, pw_ref, ls_ref, lr_ref, li_ref, u_ref, br_ref, bi_ref, sem,
):
    moves = fetch(
        (ls_hbm, lr_hbm, li_hbm, u_hbm, br_hbm, bi_hbm),
        (ls_ref, lr_ref, li_ref, u_ref, br_ref, bi_ref), sem,
    )
    for move in moves[:3]:
        move.wait()
    _, _, ar, ai = transition(lr_ref, li_ref, ls_ref)
    pr, pi = fold_groups(ar), fold_groups(ai)
    a_ref[0], a_ref[1] = pr, pi
    for _ in range(5):
        pr, pi = cmul(pr, pi, pr, pi)
    for k in range(3):
        pw_ref[2 * k], pw_ref[2 * k + 1] = pr, pi
        pr, pi = cmul(pr, pi, pr, pi)
    a_ref[2], a_ref[3] = pr, pi
    for move in moves[3:]:
        move.wait()
    put_inputs(u_ref[...], br_ref, bi_ref, xr_ref, xi_ref)

    sub = lax.broadcasted_iota(jnp.int32, (BLOCKS, HALF), 0)
    for h in range(2):
        mr = power_rows(a_ref.at[0], 8 * h, 8)
        mi = power_rows(a_ref.at[1], 8 * h, 8)

        def body(j, carried):
            hr, hi = carried
            rows = pl.ds(pl.multiple_of(j * BLOCKS, BLOCKS), BLOCKS)
            nr, ni = cmul(mr, mi, hr, hi)
            nr = nr + xr_ref[rows, pl.ds(HALF * h, HALF)]
            ni = ni + xi_ref[rows, pl.ds(HALF * h, HALF)]
            return nr, ni

        zero = jnp.zeros((BLOCKS, HALF), F32)
        er, ei = lax.fori_loop(0, STEPS, body, (zero, zero), unroll=4)
        for k in range(3):
            s = 1 << k
            qr = power_rows(pw_ref.at[2 * k], 8 * h, 8)
            qi = power_rows(pw_ref.at[2 * k + 1], 8 * h, 8)
            shr = jnp.where(sub >= s, pltpu.roll(er, s, 0), 0.0)
            shi = jnp.where(sub >= s, pltpu.roll(ei, s, 0), 0.0)
            dr, di = cmul(qr, qi, shr, shi)
            er, ei = er + dr, ei + di
        for k in range(8):
            fin_ref[pl.ds(8 * h + k, 1), :] = er[7:8, 128 * k : 128 * (k + 1)]
            fin_ref[pl.ds(16 + 8 * h + k, 1), :] = ei[7:8, 128 * k : 128 * (k + 1)]
        ent_ref[0, :, pl.ds(HALF * h, HALF)] = jnp.where(sub >= 1, pltpu.roll(er, 1, 0), 0.0)
        ent_ref[1, :, pl.ds(HALF * h, HALF)] = jnp.where(sub >= 1, pltpu.roll(ei, 1, 0), 0.0)

    fin = fin_ref[...].astype(BF16)
    for m in range(copies_ref.shape[0]):
        copies_ref[m] = fin


def spread_pairs(parts):
    left = lax.broadcasted_iota(jnp.int32, (GROUP, 128), 1) < STATE
    zero = jnp.zeros((32, 128), BF16)
    rows = []
    for k, part in enumerate(parts):
        block = jnp.concatenate([jnp.where(left, part, 0.0), jnp.where(left, 0.0, part)], axis=0)
        rows.append(jnp.concatenate([block.astype(BF16) if j == k else zero for j in range(4)], axis=1))
    return jnp.concatenate(rows, axis=0)


def local_kernel(
    ls_hbm, lr_hbm, li_hbm, cr_hbm, ci_hbm, u_hbm, br_hbm, bi_hbm, skip_hbm, a_ref, ent_ref,
    keep_ref, mine_ref, pack_ref,
    xr_ref, xi_ref, sr_ref, si_ref, y_ref,
    ls_ref, lr_ref, li_ref, cr_ref, ci_ref, u_ref, br_ref, bi_ref, skip_ref, sem,
):
    for move in fetch(
        (ls_hbm, lr_hbm, li_hbm, cr_hbm, ci_hbm, u_hbm, br_hbm, bi_hbm, skip_hbm),
        (ls_ref, lr_ref, li_ref, cr_ref, ci_ref, u_ref, br_ref, bi_ref, skip_ref), sem,
    ):
        move.wait()
    lr, li, ar, ai = transition(lr_ref, li_ref, ls_ref)
    den = lr * lr + li * li
    num = ar - 1.0
    fr = (num * lr + ai * li) / den
    fi = (ai * lr - num * li) / den
    for k in range(LB):
        pairs = []
        for g in (2 * k, 2 * k + 1):
            rows = pl.ds(GROUP * g, GROUP)
            pairs.append(cmul(cr_ref[rows, :], ci_ref[rows, :], fr[g : g + 1, :], fi[g : g + 1, :]))
        for c in range(2):
            d = jnp.concatenate([pairs[0][c], pairs[1][c]], axis=1)
            rows = pl.ds(HALF_D * c + GROUP * k, GROUP)
            mine_ref[rows, :] = d
            pack_ref[rows, :] = d
    for k in range(4):
        pack_ref[pl.ds(2 * CH + LB * k, LB), :] = a_ref[k]

    up = put_inputs(u_ref[...], br_ref, bi_ref, xr_ref, xi_ref)
    for h in range(2):
        cols = pl.ds(HALF * h, HALF)
        mr, mi = power_rows(a_ref.at[0], 8 * h, 8), power_rows(a_ref.at[1], 8 * h, 8)

        def body(j, carried):
            hr, hi = carried
            rs, ims = [], []
            for step in range(2):
                rows = pl.ds(pl.multiple_of(j * 16, 16) + 8 * step, BLOCKS)
                nr, ni = cmul(mr, mi, hr, hi)
                hr = nr + xr_ref[rows, cols]
                hi = ni + xi_ref[rows, cols]
                rs.append(hr)
                ims.append(hi)
            rows = pl.ds(pl.multiple_of(j * 16, 16), 16)
            sr_ref[rows, cols] = jnp.concatenate(rs, axis=0).astype(BF16)
            si_ref[rows, cols] = jnp.concatenate(ims, axis=0).astype(BF16)
            return hr, hi

        lax.fori_loop(0, STEPS // 2, body, (ent_ref[0, :, cols], ent_ref[1, :, cols]), unroll=2)

    for q in range(Q):
        cols = pl.ds(128 * q, 128)
        total = skip_ref[:, cols] * up[:, 128 * q : 128 * (q + 1)].astype(F32)
        for c, s_ref in enumerate((sr_ref, si_ref)):
            d = [mine_ref[pl.ds(HALF_D * c + GROUP * (4 * q + k), GROUP), :] for k in range(4)]
            wide = spread_pairs(d if c == 0 else [-part for part in d])
            total = total + lax.dot_general(
                s_ref[:, pl.ds(512 * q, 512)], wide, (((1,), (1,)), ((), ())),
                preferred_element_type=F32,
            )
        y_ref[:, cols] = total
    back = order_matrix(True)
    y = y_ref[...]
    high = y.astype(BF16)
    low = (y - high.astype(F32)).astype(BF16)
    y_ref[...] = jnp.dot(back, high, preferred_element_type=F32) + jnp.dot(
        back, low, preferred_element_type=F32
    )
    tp = lax.axis_index("tp")
    mine = pl.ds(pl.multiple_of(tp * HROWS, HROWS), HROWS)
    theirs = pl.ds(pl.multiple_of((1 - tp) * HROWS, HROWS), HROWS)
    keep_ref[...] = y_ref[mine, :]
    for q in range(Q):
        pack_ref[pl.ds(CH + HROWS * q, HROWS), :] = y_ref[theirs, pl.ds(128 * q, 128)]


def near_kernel(parts_ref, a_ref, copies_ref):
    wr, wi = a_ref[2], a_ref[3]
    index = near_index()
    plane = lax.axis_index("z")
    tr, ti = jnp.zeros((LB, 128), F32), jnp.zeros((LB, 128), F32)
    br, bi = tr, ti
    for k in range(parts_ref.shape[0]):
        here = index == k
        br, bi = jnp.where(here, tr, br), jnp.where(here, ti, bi)
        part = parts_ref[k].astype(F32)
        mr, mi = cmul(wr, wi, tr, ti)
        tr, ti = mr + part[:LB], mi + part[LB:]
    total = jnp.concatenate([tr, ti], axis=0).astype(BF16)
    before = jnp.concatenate([br, bi], axis=0).astype(BF16)
    for m in range(copies_ref.shape[0]):
        copies_ref[m] = jnp.where(plane == m // 2, before, total)


def load_kernel(w_hbm, w_ref, sem):
    move = pltpu.make_async_copy(w_hbm, w_ref, sem.at[0])
    move.start()
    move.wait()


def power_tables(o, base, whole, tr_ref, ti_ref, pw_ref, a_ref):
    near, tp = near_index(), lax.axis_index("tp")
    sub = lax.broadcasted_iota(jnp.int32, (BLOCKS, HALF), 0)
    pr, pi = whole
    ir, ii = jnp.ones((LB, 128), F32), jnp.zeros((LB, 128), F32)
    for k in range(5):
        bit = ((near >> k) & 1) == 1
        jr, ji = cmul(ir, ii, pr, pi)
        ir, ii = jnp.where(bit, jr, ir), jnp.where(bit, ji, ii)
        pr, pi = cmul(pr, pi, pr, pi)
    pw_ref[o, 0], pw_ref[o, 1], pw_ref[o, 2], pw_ref[o, 3] = ir, ii, pr, pi
    pr, pi = base
    for k in range(8):
        a_ref[2 * k], a_ref[2 * k + 1] = pr, pi
        pr, pi = cmul(pr, pi, pr, pi)
    for h in range(2):
        cols = pl.ds(HALF * h, HALF)

        def power(k):
            return power_rows(a_ref.at[2 * k], 8 * h, 8), power_rows(a_ref.at[2 * k + 1], 8 * h, 8)

        mr, mi = power(0)
        for k, bit in ((0, (sub & 1) != 0), (1, (sub & 2) != 0), (2, (sub & 4) != 0), (7, tp == 1)):
            qr, qi = power(k)
            jr, ji = cmul(mr, mi, qr, qi)
            mr, mi = jnp.where(bit, jr, mr), jnp.where(bit, ji, mi)
        er, ei = power(3)

        def body(j, carried):
            hr, hi = carried
            nr, ni = cmul(er, ei, hr, hi)
            rows = pl.ds(pl.multiple_of(j * 16, 16), 16)
            tr_ref[o, rows, cols] = jnp.concatenate([hr, nr], axis=0).astype(BF16)
            ti_ref[o, rows, cols] = jnp.concatenate([hi, ni], axis=0).astype(BF16)
            return cmul(er, ei, nr, ni)

        lax.fori_loop(0, HROWS // 16, body, (mr, mi))


def gelu(x):
    return 0.5 * x * (1.0 + jnp.tanh(0.7978845608028654 * (x + 0.044715 * (x * x * x))))


def last_kernel(
    parts_ref, keep_ref, mine_ref, other_ref, powers_ref, vw_ref,
    gw_hbm, vo_hbm, go_hbm, vb_hbm, gb_hbm,
    out_hbm,
    in_ref, act_ref, out_ref, w_ref, vb_ref, gb_ref, tr_ref, ti_ref, pw_ref, a_ref, sem,
):
    width = out_ref.shape[1]
    chunks = width // CHUNK
    moves, results = [], []
    for n in range(chunks):
        cols = pl.ds(CHUNK * n, CHUNK)
        for k, w_hbm in enumerate((vo_hbm, gw_hbm, go_hbm)):
            moves.append(pltpu.make_async_copy(w_hbm.at[:, cols], w_ref.at[k, :, cols], sem.at[3 * n + k]))
    biases = [
        pltpu.make_async_copy(vb_hbm, vb_ref, sem.at[3 * chunks]),
        pltpu.make_async_copy(gb_hbm, gb_ref, sem.at[3 * chunks + 1]),
    ]
    for move in biases + moves:
        move.start()

    for o in range(2):
        both = [powers_ref[k] if o == 0 else other_ref[pl.ds(2 * CH + LB * k, LB), :] for k in range(4)]
        power_tables(o, both[:2], both[2:], tr_ref, ti_ref, pw_ref, a_ref)

    far, tp = lax.axis_index("z"), lax.axis_index("tp")
    n_far = parts_ref.shape[0] // 2
    for o in range(2):
        side = tp if o == 0 else 1 - tp
        wr, wi = pw_ref[o, 2], pw_ref[o, 3]
        gr, gi = jnp.zeros((LB, 128), F32), jnp.zeros((LB, 128), F32)
        for k in range(n_far - 1):
            part = parts_ref[2 * k + side].astype(F32)
            mr, mi = cmul(wr, wi, gr, gi)
            gr = jnp.where(k < far, mr + part[:LB], gr)
            gi = jnp.where(k < far, mi + part[LB:], gi)
        before = parts_ref[2 * far + side].astype(F32)
        mr, mi = cmul(pw_ref[o, 0], pw_ref[o, 1], gr, gi)
        in_ref[2 * o], in_ref[2 * o + 1] = before[:LB] + mr, before[LB:] + mi

    for o, d_ref in enumerate((mine_ref, other_ref)):
        for q in range(Q):
            real, imag = [], []
            for k in range(4 * q, 4 * q + 4):
                vr, vi = cmul(
                    d_ref[pl.ds(GROUP * k, GROUP), :], d_ref[pl.ds(HALF_D + GROUP * k, GROUP), :],
                    in_ref[2 * o, pl.ds(k, 1), :], in_ref[2 * o + 1, pl.ds(k, 1), :],
                )
                real.append(vr)
                imag.append(-vi)
            cols = pl.ds(128 * q, 128)
            total = keep_ref[:, cols] if o == 0 else other_ref[pl.ds(CH + HROWS * q, HROWS), :]
            for v, t_ref in ((real, tr_ref), (imag, ti_ref)):
                total = total + lax.dot_general(
                    t_ref[o, :, pl.ds(512 * q, 512)], spread_pairs(v), (((1,), (1,)), ((), ())),
                    preferred_element_type=F32,
                )
            act_ref[o, :, cols] = gelu(total).astype(BF16)

    def product(o, k, cols):
        w = vw_ref[:, cols] if k < 0 else w_ref[k, :, cols]
        return jnp.dot(act_ref[o], w, preferred_element_type=F32).astype(BF16).astype(F32)

    for move in biases:
        move.wait()
    for n in range(chunks):
        cols = pl.ds(CHUNK * n, CHUNK)
        for move in moves[3 * n : 3 * n + 3]:
            move.wait()
        value = product(0, -1, cols) + product(1, 0, cols) + vb_ref[:, cols]
        gate = product(0, 1, cols) + product(1, 2, cols) + gb_ref[:, cols]
        out_ref[:, cols] = (value * jax.nn.sigmoid(gate)).astype(BF16)
        results.append(
            pltpu.make_async_copy(out_ref.at[:, cols], out_hbm.at[:, cols], sem.at[3 * chunks + 2 + n])
        )
        results[-1].start()
    for move in results:
        move.wait()


def call(kernel, outs, ins, scratch=(), limit=16):
    fn = pl.pallas_call(
        kernel,
        out_shape=[VMEM(s, d) if v else jax.ShapeDtypeStruct(s, d) for s, d, v in outs],
        in_specs=[pl.BlockSpec(memory_space=VMEM if m is True else m) for m in ins],
        out_specs=[pl.BlockSpec(memory_space=pltpu.HBM if v is None else VMEM) for _, _, v in outs],
        scratch_shapes=list(scratch),
        compiler_params=pltpu.CompilerParams(vmem_limit_bytes=limit * 1024 * 1024),
    )

    def run(*args):
        placed = []
        for a, m in zip(args, ins, strict=True):
            if m is True:
                a = pltpu.with_memory_space_constraint(a, VMEM)
            elif m is pltpu.HBM:
                a = pltpu.with_memory_space_constraint(a, pltpu.HBM)
            placed.append(a)
        return fn(*placed)

    return run


def to_all(copies, axes):
    return lax.all_to_all(copies, axes, split_axis=0, concat_axis=0, tiled=True)


def mixer(
    features, lambda_real, lambda_imag, log_step, input_real, input_imag, real_output,
    imaginary_output, skip_gain, value_weight, gate_weight, value_bias, gate_bias,
):
    n_near = lax.axis_size("y") * lax.axis_size("x")
    n_far = lax.axis_size("z")
    smem, hbm = pltpu.SMEM, pltpu.HBM
    width = value_weight.shape[1]
    b_re = input_real.transpose(0, 2, 1).reshape(CH, STATE)
    b_im = input_imag.transpose(0, 2, 1).reshape(CH, STATE)
    params = (log_step, lambda_real, lambda_imag, b_re, b_im)
    rates = [smem((G,), F32), VMEM((G, STATE), F32), VMEM((G, STATE), F32)]
    matrix = [VMEM((CH, STATE), F32), VMEM((CH, STATE), F32)]

    copies, powers, entering = call(
        first_kernel,
        [((n_near, 32, 128), BF16, True), ((4, LB, 128), F32, True), ((2, BLOCKS, FLAT), F32, True)],
        [hbm] * 6,
        [
            VMEM((T, FLAT), F32), VMEM((T, FLAT), F32), VMEM((32, 128), F32), VMEM((6, LB, 128), F32),
            *rates, VMEM((T, CH), BF16), *matrix, pltpu.SemaphoreType.DMA((6,)),
        ],
        16,
    )(*params[:3], features, *params[3:])
    parts = to_all(copies, NEAR)
    local_call = call(
        local_kernel,
        [((HROWS, CH), F32, True), ((CH, 128), F32, True), ((PACK, 128), F32, False)],
        [hbm] * 9 + [True, True],
        [
            VMEM((T, FLAT), F32), VMEM((T, FLAT), F32), VMEM((T, FLAT), BF16), VMEM((T, FLAT), BF16),
            VMEM((T, CH), F32), *rates, *matrix, VMEM((T, CH), BF16), *matrix, VMEM((1, CH), F32),
            pltpu.SemaphoreType.DMA((9,)),
        ],
        20,
    )
    keep, mine, pack = local_call(
        *params[:3], real_output.reshape(CH, STATE), imaginary_output.reshape(CH, STATE),
        features, *params[3:], skip_gain.reshape(1, CH), powers, entering,
    )
    value_other = lax.ppermute(value_weight, "tp", SWAP)
    gate_other = lax.ppermute(gate_weight, "tp", SWAP)
    pack_other = lax.ppermute(pack, "tp", SWAP)
    near_call = call(near_kernel, [((2 * n_far, 32, 128), BF16, True)], [True, True], limit=4)
    (totals,) = near_call(parts, powers)
    planes = to_all(totals, FAR)
    load_call = call(load_kernel, [((CH, width), BF16, True)], [hbm], [pltpu.SemaphoreType.DMA((1,))], 4)
    (value_near,) = load_call(value_weight)
    (out,) = call(
        last_kernel,
        [((HROWS, width), BF16, None)],
        [True] * 6 + [hbm] * 5,
        [
            VMEM((4, LB, 128), F32), VMEM((2, HROWS, CH), BF16), VMEM((HROWS, width), BF16),
            VMEM((3, CH, width), BF16),
            VMEM((1, width), F32), VMEM((1, width), F32),
            VMEM((2, HROWS, FLAT), BF16), VMEM((2, HROWS, FLAT), BF16), VMEM((2, 4, LB, 128), F32),
            VMEM((16, LB, 128), F32), pltpu.SemaphoreType.DMA((4 * (width // CHUNK) + 2,)),
        ],
        24,
    )(
        planes, keep, mine, pack_other, powers, value_near, gate_weight, value_other, gate_other,
        value_bias.reshape(1, width), gate_bias.reshape(1, width),
    )
    return out


def solution(mesh):
    split = Mesh(mesh.devices.reshape(8, 8, 4, mesh.shape["tp"]), SP_TP)
    in_specs = (
        P(SP, "tp"),
        P("tp", None),
        P("tp", None),
        P("tp"),
        P("tp", None, None),
        P("tp", None, None),
        P("tp", None, None),
        P("tp", None, None),
        P("tp"),
        P("tp", None),
        P("tp", None),
        P(),
        P(),
    )
    return jax.shard_map(mixer, mesh=split, in_specs=in_specs, out_specs=P(SP_TP, None), check_vma=False)
```

```python
import jax
import jax.numpy as jnp
from jax import lax
from jax.experimental import pallas as pl
from jax.experimental.pallas import tpu as pltpu
from jax.sharding import Mesh
from jax.sharding import PartitionSpec as P

SP = ("z", "y", "x")
SP_TP = ("z", "y", "x", "tp")
NEAR = ("y", "x")
FAR = ("z", "tp")
SWAP = [(0, 1), (1, 0)]

T = 256
BLOCKS = 8
STEPS = 32
SKIP = 4
G = 32
STATE = 64
GROUP = 16
CH = 512
FLAT = 2048
LB = 16
HALF = 1024
Q = 4
HROWS = 128
HALF_D = CH // 2
PACK = 2 * CH + 4 * LB
CHUNK = 1024

F32 = jnp.float32
BF16 = jnp.bfloat16
VMEM = pltpu.VMEM


def cmul(ar, ai, br, bi):
    return ar * br - ai * bi, ar * bi + ai * br


def power_rows(a_ref, lo, n):
    return jnp.concatenate(
        [jnp.broadcast_to(a_ref[pl.ds(lo + k, 1), :], (BLOCKS, 128)) for k in range(n)], axis=1
    )


def transition(lr_ref, li_ref, ls_ref):
    row = lax.broadcasted_iota(jnp.int32, (G, STATE), 0)
    logs = jnp.zeros((G, STATE), F32)
    for g in range(G):
        logs = jnp.where(row == g, ls_ref[g], logs)
    step = jnp.exp(logs)
    lr = lr_ref[...]
    li = li_ref[...]
    magnitude = jnp.exp(lr * step)
    phase = li * step
    return lr, li, magnitude * jnp.cos(phase), magnitude * jnp.sin(phase)


def order_matrix(transposed):
    r = lax.broadcasted_iota(jnp.int32, (T, T), 1 if transposed else 0)
    t = lax.broadcasted_iota(jnp.int32, (T, T), 0 if transposed else 1)
    hit = t == (r & 7) * STEPS + (r >> 3)
    return jnp.where(hit, 1.0, 0.0).astype(BF16)


def fold_groups(a):
    row = lax.broadcasted_iota(jnp.int32, (LB, G), 0)
    col = lax.broadcasted_iota(jnp.int32, (LB, G), 1)
    even = jnp.where(col == 2 * row, 1.0, 0.0)
    odd = jnp.where(col == 2 * row + 1, 1.0, 0.0)
    hi = lax.Precision.HIGHEST
    left = jnp.dot(even, a, precision=hi, preferred_element_type=F32)
    right = jnp.dot(odd, a, precision=hi, preferred_element_type=F32)
    return jnp.concatenate([left, right], axis=1)


def near_index():
    return lax.axis_index("y") * lax.axis_size("x") + lax.axis_index("x")


def spread_pairs(parts):
    lane = lax.broadcasted_iota(jnp.int32, (GROUP, 128), 1)
    left = jnp.where(lane < STATE, 1.0, 0.0).astype(BF16)
    right = jnp.where(lane < STATE, 0.0, 1.0).astype(BF16)
    zero = jnp.zeros((32, 128), BF16)
    rows = []
    for k, part in enumerate(parts):
        part = part.astype(BF16)
        block = jnp.concatenate([part * left, part * right], axis=0)
        rows.append(jnp.concatenate([block if j == k else zero for j in range(4)], axis=1))
    return jnp.concatenate(rows, axis=0)


def paired(ref, k):
    at = 2 * GROUP * k
    return jnp.concatenate([ref[pl.ds(at, GROUP), :], ref[pl.ds(at + GROUP, GROUP), :]], axis=1)


def put_inputs(u, br_ref, bi_ref, xr_ref, xi_ref):
    up = jnp.dot(order_matrix(False), u, preferred_element_type=F32).astype(BF16)
    for q in range(Q):
        for b_ref, x_ref in ((br_ref, xr_ref), (bi_ref, xi_ref)):
            wide = spread_pairs([paired(b_ref, 4 * q + k) for k in range(4)])
            x_ref[:, pl.ds(512 * q, 512)] = jnp.dot(
                up[:, 128 * q : 128 * (q + 1)], wide, preferred_element_type=F32
            )
    return up


def fetch(sources, targets, sem):
    moves = [
        pltpu.make_async_copy(src, dst, sem.at[k])
        for k, (src, dst) in enumerate(zip(sources, targets, strict=True))
    ]
    for move in moves:
        move.start()
    return moves


def first_kernel(
    ls_hbm, lr_hbm, li_hbm, u_hbm, br_hbm, bi_hbm,
    copies_ref, a_ref, ent_ref,
    xr_ref, xi_ref, fin_ref, pw_ref, step_ref, ls_ref, lr_ref, li_ref, u_ref, br_ref, bi_ref, sem,
):
    moves = fetch(
        (ls_hbm, lr_hbm, li_hbm, u_hbm, br_hbm, bi_hbm),
        (ls_ref, lr_ref, li_ref, u_ref, br_ref, bi_ref), sem,
    )
    for move in moves[:3]:
        move.wait()
    _, _, ar, ai = transition(lr_ref, li_ref, ls_ref)
    pr, pi = fold_groups(ar), fold_groups(ai)
    a_ref[0], a_ref[1] = pr, pi
    step_ref[0], step_ref[1] = pr, pi
    qr, qi = cmul(pr, pi, pr, pi)
    step_ref[2], step_ref[3] = qr, qi
    step_ref[4], step_ref[5] = cmul(pr, pi, qr, qi)
    pr, pi = cmul(qr, qi, qr, qi)
    step_ref[6], step_ref[7] = pr, pi
    for _ in range(3):
        pr, pi = cmul(pr, pi, pr, pi)
    for k in range(3):
        pw_ref[2 * k], pw_ref[2 * k + 1] = pr, pi
        pr, pi = cmul(pr, pi, pr, pi)
    a_ref[2], a_ref[3] = pr, pi
    for move in moves[3:]:
        move.wait()
    row = lax.broadcasted_iota(jnp.int32, (T, T), 0)
    col = lax.broadcasted_iota(jnp.int32, (T, T), 1)
    hit = col == (row & 7) * STEPS + ((row >> 3) & 7) * SKIP + (row >> 6)
    up = jnp.dot(
        jnp.where(hit, 1.0, 0.0).astype(BF16), u_ref[...], preferred_element_type=F32
    ).astype(BF16)
    for q in range(Q):
        cols = slice(128 * q, 128 * (q + 1))
        left = jnp.concatenate([up[64 * s : 64 * (s + 1), cols] for s in range(SKIP)], axis=1)
        real, imag = [[] for _ in range(SKIP)], [[] for _ in range(SKIP)]
        for k in range(4 * q, 4 * q + 4):
            b_re, b_im = paired(br_ref, k), paired(bi_ref, k)
            for s in range(SKIP):
                if s == SKIP - 1:
                    vr, vi = b_re, b_im
                else:
                    n = 2 * (SKIP - 2 - s)
                    vr, vi = cmul(step_ref[n, pl.ds(k, 1), :], step_ref[n + 1, pl.ds(k, 1), :], b_re, b_im)
                real[s].append(vr)
                imag[s].append(vi)
        for v, x_ref in ((real, xr_ref), (imag, xi_ref)):
            right = jnp.concatenate([spread_pairs(parts) for parts in v], axis=0)
            x_ref[:, pl.ds(512 * q, 512)] = jnp.dot(left, right, preferred_element_type=F32)

    sub = lax.broadcasted_iota(jnp.int32, (BLOCKS, HALF), 0)
    for h in range(2):
        mr = power_rows(step_ref.at[6], 8 * h, 8)
        mi = power_rows(step_ref.at[7], 8 * h, 8)
        cols = pl.ds(HALF * h, HALF)
        er, ei = xr_ref[pl.ds(0, BLOCKS), cols], xi_ref[pl.ds(0, BLOCKS), cols]
        for j in range(1, STEPS // SKIP):
            rows = pl.ds(BLOCKS * j, BLOCKS)
            er, ei = cmul(mr, mi, er, ei)
            er = er + xr_ref[rows, cols]
            ei = ei + xi_ref[rows, cols]
        for k in range(3):
            s = 1 << k
            qr = power_rows(pw_ref.at[2 * k], 8 * h, 8)
            qi = power_rows(pw_ref.at[2 * k + 1], 8 * h, 8)
            shr = jnp.where(sub >= s, pltpu.roll(er, s, 0), 0.0)
            shi = jnp.where(sub >= s, pltpu.roll(ei, s, 0), 0.0)
            dr, di = cmul(qr, qi, shr, shi)
            er, ei = er + dr, ei + di
        for k in range(8):
            fin_ref[pl.ds(8 * h + k, 1), :] = er[7:8, 128 * k : 128 * (k + 1)]
            fin_ref[pl.ds(16 + 8 * h + k, 1), :] = ei[7:8, 128 * k : 128 * (k + 1)]
        ent_ref[0, :, pl.ds(HALF * h, HALF)] = jnp.where(sub >= 1, pltpu.roll(er, 1, 0), 0.0)
        ent_ref[1, :, pl.ds(HALF * h, HALF)] = jnp.where(sub >= 1, pltpu.roll(ei, 1, 0), 0.0)

    fin = fin_ref[...].astype(BF16)
    for m in range(copies_ref.shape[0]):
        copies_ref[m] = fin


def local_kernel(
    ls_hbm, lr_hbm, li_hbm, cr_hbm, ci_hbm, u_hbm, br_hbm, bi_hbm, skip_hbm, a_ref, ent_ref,
    keep_ref, mine_ref, pack_ref,
    xr_ref, xi_ref, sr_ref, si_ref, y_ref,
    ls_ref, lr_ref, li_ref, cr_ref, ci_ref, u_ref, br_ref, bi_ref, skip_ref, sem,
):
    for move in fetch(
        (ls_hbm, lr_hbm, li_hbm, cr_hbm, ci_hbm, u_hbm, br_hbm, bi_hbm, skip_hbm),
        (ls_ref, lr_ref, li_ref, cr_ref, ci_ref, u_ref, br_ref, bi_ref, skip_ref), sem,
    ):
        move.wait()
    lr, li, ar, ai = transition(lr_ref, li_ref, ls_ref)
    den = lr * lr + li * li
    num = ar - 1.0
    fr = (num * lr + ai * li) / den
    fi = (ai * lr - num * li) / den
    for k in range(LB):
        pairs = []
        for g in (2 * k, 2 * k + 1):
            rows = pl.ds(GROUP * g, GROUP)
            pairs.append(cmul(cr_ref[rows, :], ci_ref[rows, :], fr[g : g + 1, :], fi[g : g + 1, :]))
        for c in range(2):
            d = jnp.concatenate([pairs[0][c], pairs[1][c]], axis=1)
            rows = pl.ds(HALF_D * c + GROUP * k, GROUP)
            mine_ref[rows, :] = d
            pack_ref[rows, :] = d
    for k in range(4):
        pack_ref[pl.ds(2 * CH + LB * k, LB), :] = a_ref[k]

    up = put_inputs(u_ref[...], br_ref, bi_ref, xr_ref, xi_ref)
    for h in range(2):
        cols = pl.ds(HALF * h, HALF)
        mr, mi = power_rows(a_ref.at[0], 8 * h, 8), power_rows(a_ref.at[1], 8 * h, 8)

        def body(j, carried):
            hr, hi = carried
            rs, ims = [], []
            for step in range(2):
                rows = pl.ds(pl.multiple_of(j * 16, 16) + 8 * step, BLOCKS)
                nr, ni = cmul(mr, mi, hr, hi)
                hr = nr + xr_ref[rows, cols]
                hi = ni + xi_ref[rows, cols]
                rs.append(hr)
                ims.append(hi)
            rows = pl.ds(pl.multiple_of(j * 16, 16), 16)
            sr_ref[rows, cols] = jnp.concatenate(rs, axis=0).astype(BF16)
            si_ref[rows, cols] = jnp.concatenate(ims, axis=0).astype(BF16)
            return hr, hi

        lax.fori_loop(0, STEPS // 2, body, (ent_ref[0, :, cols], ent_ref[1, :, cols]), unroll=2)

    for q in range(Q):
        cols = pl.ds(128 * q, 128)
        total = skip_ref[:, cols] * up[:, 128 * q : 128 * (q + 1)].astype(F32)
        for c, s_ref in enumerate((sr_ref, si_ref)):
            d = [mine_ref[pl.ds(HALF_D * c + GROUP * (4 * q + k), GROUP), :] for k in range(4)]
            wide = spread_pairs(d if c == 0 else [-part for part in d])
            total = total + lax.dot_general(
                s_ref[:, pl.ds(512 * q, 512)], wide, (((1,), (1,)), ((), ())),
                preferred_element_type=F32,
            )
        y_ref[:, cols] = total
    back = order_matrix(True)
    y = y_ref[...]
    high = y.astype(BF16)
    low = (y - high.astype(F32)).astype(BF16)
    y_ref[...] = jnp.dot(back, high, preferred_element_type=F32) + jnp.dot(
        back, low, preferred_element_type=F32
    )
    tp = lax.axis_index("tp")
    mine = pl.ds(pl.multiple_of(tp * HROWS, HROWS), HROWS)
    theirs = pl.ds(pl.multiple_of((1 - tp) * HROWS, HROWS), HROWS)
    keep_ref[...] = y_ref[mine, :]
    for q in range(Q):
        pack_ref[pl.ds(CH + HROWS * q, HROWS), :] = y_ref[theirs, pl.ds(128 * q, 128)]


def near_kernel(parts_ref, a_ref, copies_ref):
    wr, wi = a_ref[2], a_ref[3]
    index = near_index()
    plane = lax.axis_index("z")
    tr, ti = jnp.zeros((LB, 128), F32), jnp.zeros((LB, 128), F32)
    br, bi = tr, ti
    for k in range(parts_ref.shape[0]):
        here = index == k
        br, bi = jnp.where(here, tr, br), jnp.where(here, ti, bi)
        part = parts_ref[k].astype(F32)
        mr, mi = cmul(wr, wi, tr, ti)
        tr, ti = mr + part[:LB], mi + part[LB:]
    total = jnp.concatenate([tr, ti], axis=0).astype(BF16)
    before = jnp.concatenate([br, bi], axis=0).astype(BF16)
    for m in range(copies_ref.shape[0]):
        copies_ref[m] = jnp.where(plane == m // 2, before, total)


def load_kernel(w_hbm, w_ref, sem):
    move = pltpu.make_async_copy(w_hbm, w_ref, sem.at[0])
    move.start()
    move.wait()


def power_tables(o, base, whole, tr_ref, ti_ref, pw_ref, a_ref):
    near, tp = near_index(), lax.axis_index("tp")
    sub = lax.broadcasted_iota(jnp.int32, (BLOCKS, HALF), 0)
    pr, pi = whole
    ir, ii = jnp.ones((LB, 128), F32), jnp.zeros((LB, 128), F32)
    for k in range(5):
        bit = ((near >> k) & 1) == 1
        jr, ji = cmul(ir, ii, pr, pi)
        ir, ii = jnp.where(bit, jr, ir), jnp.where(bit, ji, ii)
        pr, pi = cmul(pr, pi, pr, pi)
    pw_ref[o, 0], pw_ref[o, 1], pw_ref[o, 2], pw_ref[o, 3] = ir, ii, pr, pi
    pr, pi = base
    for k in range(8):
        a_ref[2 * k], a_ref[2 * k + 1] = pr, pi
        pr, pi = cmul(pr, pi, pr, pi)
    for h in range(2):
        cols = pl.ds(HALF * h, HALF)

        def power(k):
            return power_rows(a_ref.at[2 * k], 8 * h, 8), power_rows(a_ref.at[2 * k + 1], 8 * h, 8)

        mr, mi = power(0)
        for k, bit in ((0, (sub & 1) != 0), (1, (sub & 2) != 0), (2, (sub & 4) != 0), (7, tp == 1)):
            qr, qi = power(k)
            jr, ji = cmul(mr, mi, qr, qi)
            mr, mi = jnp.where(bit, jr, mr), jnp.where(bit, ji, mi)
        er, ei = power(3)

        def body(j, carried):
            hr, hi = carried
            nr, ni = cmul(er, ei, hr, hi)
            rows = pl.ds(pl.multiple_of(j * 16, 16), 16)
            tr_ref[o, rows, cols] = jnp.concatenate([hr, nr], axis=0).astype(BF16)
            ti_ref[o, rows, cols] = jnp.concatenate([hi, ni], axis=0).astype(BF16)
            return cmul(er, ei, nr, ni)

        lax.fori_loop(0, HROWS // 16, body, (mr, mi))


def gelu(x):
    return 0.5 * x * (1.0 + jnp.tanh(0.7978845608028654 * (x + 0.044715 * (x * x * x))))


def last_kernel(
    parts_ref, keep_ref, mine_ref, other_ref, powers_ref, vw_ref,
    gw_hbm, vo_hbm, go_hbm, vb_hbm, gb_hbm,
    out_hbm,
    in_ref, act_ref, out_ref, w_ref, vb_ref, gb_ref, tr_ref, ti_ref, pw_ref, a_ref, sem,
):
    width = out_ref.shape[1]
    chunks = width // CHUNK
    moves, results = [], []
    for n in range(chunks):
        cols = pl.ds(CHUNK * n, CHUNK)
        for k, w_hbm in enumerate((vo_hbm, gw_hbm, go_hbm)):
            moves.append(pltpu.make_async_copy(w_hbm.at[:, cols], w_ref.at[k, :, cols], sem.at[3 * n + k]))
    biases = [
        pltpu.make_async_copy(vb_hbm, vb_ref, sem.at[3 * chunks]),
        pltpu.make_async_copy(gb_hbm, gb_ref, sem.at[3 * chunks + 1]),
    ]
    for move in biases + moves:
        move.start()

    for o in range(2):
        both = [powers_ref[k] if o == 0 else other_ref[pl.ds(2 * CH + LB * k, LB), :] for k in range(4)]
        power_tables(o, both[:2], both[2:], tr_ref, ti_ref, pw_ref, a_ref)

    far, tp = lax.axis_index("z"), lax.axis_index("tp")
    n_far = parts_ref.shape[0] // 2
    for o in range(2):
        side = tp if o == 0 else 1 - tp
        wr, wi = pw_ref[o, 2], pw_ref[o, 3]
        gr, gi = jnp.zeros((LB, 128), F32), jnp.zeros((LB, 128), F32)
        for k in range(n_far - 1):
            part = parts_ref[2 * k + side].astype(F32)
            mr, mi = cmul(wr, wi, gr, gi)
            gr = jnp.where(k < far, mr + part[:LB], gr)
            gi = jnp.where(k < far, mi + part[LB:], gi)
        before = parts_ref[2 * far + side].astype(F32)
        mr, mi = cmul(pw_ref[o, 0], pw_ref[o, 1], gr, gi)
        in_ref[2 * o], in_ref[2 * o + 1] = before[:LB] + mr, before[LB:] + mi

    for o, d_ref in enumerate((mine_ref, other_ref)):
        for q in range(Q):
            real, imag = [], []
            for k in range(4 * q, 4 * q + 4):
                vr, vi = cmul(
                    d_ref[pl.ds(GROUP * k, GROUP), :], d_ref[pl.ds(HALF_D + GROUP * k, GROUP), :],
                    in_ref[2 * o, pl.ds(k, 1), :], in_ref[2 * o + 1, pl.ds(k, 1), :],
                )
                real.append(vr)
                imag.append(-vi)
            cols = pl.ds(128 * q, 128)
            total = keep_ref[:, cols] if o == 0 else other_ref[pl.ds(CH + HROWS * q, HROWS), :]
            for v, t_ref in ((real, tr_ref), (imag, ti_ref)):
                total = total + lax.dot_general(
                    t_ref[o, :, pl.ds(512 * q, 512)], spread_pairs(v), (((1,), (1,)), ((), ())),
                    preferred_element_type=F32,
                )
            act_ref[o, :, cols] = gelu(total).astype(BF16)

    def product(o, k, cols):
        w = vw_ref[:, cols] if k < 0 else w_ref[k, :, cols]
        return jnp.dot(act_ref[o], w, preferred_element_type=F32).astype(BF16).astype(F32)

    for move in biases:
        move.wait()
    for n in range(chunks):
        cols = pl.ds(CHUNK * n, CHUNK)
        for move in moves[3 * n : 3 * n + 3]:
            move.wait()
        value = product(0, -1, cols) + product(1, 0, cols) + vb_ref[:, cols]
        gate = product(0, 1, cols) + product(1, 2, cols) + gb_ref[:, cols]
        out_ref[:, cols] = (value * jax.nn.sigmoid(gate)).astype(BF16)
        results.append(
            pltpu.make_async_copy(out_ref.at[:, cols], out_hbm.at[:, cols], sem.at[3 * chunks + 2 + n])
        )
        results[-1].start()
    for move in results:
        move.wait()


def call(kernel, outs, ins, scratch=(), limit=16):
    fn = pl.pallas_call(
        kernel,
        out_shape=[VMEM(s, d) if v else jax.ShapeDtypeStruct(s, d) for s, d, v in outs],
        in_specs=[pl.BlockSpec(memory_space=VMEM if m is True else m) for m in ins],
        out_specs=[pl.BlockSpec(memory_space=pltpu.HBM if v is None else VMEM) for _, _, v in outs],
        scratch_shapes=list(scratch),
        compiler_params=pltpu.CompilerParams(vmem_limit_bytes=limit * 1024 * 1024),
    )

    def run(*args):
        placed = []
        for a, m in zip(args, ins, strict=True):
            if m is True:
                a = pltpu.with_memory_space_constraint(a, VMEM)
            elif m is pltpu.HBM:
                a = pltpu.with_memory_space_constraint(a, pltpu.HBM)
            placed.append(a)
        return fn(*placed)

    return run


def to_all(copies, axes):
    return lax.all_to_all(copies, axes, split_axis=0, concat_axis=0, tiled=True)


def mixer(
    features, lambda_real, lambda_imag, log_step, input_real, input_imag, real_output,
    imaginary_output, skip_gain, value_weight, gate_weight, value_bias, gate_bias,
):
    n_near = lax.axis_size("y") * lax.axis_size("x")
    n_far = lax.axis_size("z")
    smem, hbm = pltpu.SMEM, pltpu.HBM
    width = value_weight.shape[1]
    b_re = input_real.transpose(0, 2, 1).reshape(CH, STATE)
    b_im = input_imag.transpose(0, 2, 1).reshape(CH, STATE)
    params = (log_step, lambda_real, lambda_imag, b_re, b_im)
    rates = [smem((G,), F32), VMEM((G, STATE), F32), VMEM((G, STATE), F32)]
    matrix = [VMEM((CH, STATE), F32), VMEM((CH, STATE), F32)]

    copies, powers, entering = call(
        first_kernel,
        [((n_near, 32, 128), BF16, True), ((4, LB, 128), F32, True), ((2, BLOCKS, FLAT), F32, True)],
        [hbm] * 6,
        [
            VMEM((T // SKIP, FLAT), F32), VMEM((T // SKIP, FLAT), F32), VMEM((32, 128), F32),
            VMEM((6, LB, 128), F32), VMEM((8, LB, 128), F32),
            *rates, VMEM((T, CH), BF16), *matrix, pltpu.SemaphoreType.DMA((6,)),
        ],
        16,
    )(*params[:3], features, *params[3:])
    parts = to_all(copies, NEAR)
    local_call = call(
        local_kernel,
        [((HROWS, CH), F32, True), ((CH, 128), F32, True), ((PACK, 128), F32, False)],
        [hbm] * 9 + [True, True],
        [
            VMEM((T, FLAT), F32), VMEM((T, FLAT), F32), VMEM((T, FLAT), BF16), VMEM((T, FLAT), BF16),
            VMEM((T, CH), F32), *rates, *matrix, VMEM((T, CH), BF16), *matrix, VMEM((1, CH), F32),
            pltpu.SemaphoreType.DMA((9,)),
        ],
        20,
    )
    keep, mine, pack = local_call(
        *params[:3], real_output.reshape(CH, STATE), imaginary_output.reshape(CH, STATE),
        features, *params[3:], skip_gain.reshape(1, CH), powers, entering,
    )
    value_other = lax.ppermute(value_weight, "tp", SWAP)
    gate_other = lax.ppermute(gate_weight, "tp", SWAP)
    pack_other = lax.ppermute(pack, "tp", SWAP)
    near_call = call(near_kernel, [((2 * n_far, 32, 128), BF16, True)], [True, True], limit=4)
    (totals,) = near_call(parts, powers)
    planes = to_all(totals, FAR)
    load_call = call(
        load_kernel, [((CH, width), BF16, True)], [hbm], [pltpu.SemaphoreType.DMA((1,))], 4
    )
    (value_near,) = load_call(value_weight)
    (out,) = call(
        last_kernel,
        [((HROWS, width), BF16, None)],
        [True] * 6 + [hbm] * 5,
        [
            VMEM((4, LB, 128), F32), VMEM((2, HROWS, CH), BF16), VMEM((HROWS, width), BF16),
            VMEM((3, CH, width), BF16),
            VMEM((1, width), F32), VMEM((1, width), F32),
            VMEM((2, HROWS, FLAT), BF16), VMEM((2, HROWS, FLAT), BF16), VMEM((2, 4, LB, 128), F32),
            VMEM((16, LB, 128), F32), pltpu.SemaphoreType.DMA((4 * (width // CHUNK) + 2,)),
        ],
        24,
    )(
        planes, keep, mine, pack_other, powers, value_near, gate_weight, value_other, gate_other,
        value_bias.reshape(1, width), gate_bias.reshape(1, width),
    )
    return out


def solution(mesh):
    split = Mesh(mesh.devices.reshape(8, 8, 4, mesh.shape["tp"]), SP_TP)
    in_specs = (
        P(SP, "tp"),
        P("tp", None),
        P("tp", None),
        P("tp"),
        P("tp", None, None),
        P("tp", None, None),
        P("tp", None, None),
        P("tp", None, None),
        P("tp"),
        P("tp", None),
        P("tp", None),
        P(),
        P(),
    )
    return jax.shard_map(mixer, mesh=split, in_specs=in_specs, out_specs=P(SP_TP, None), check_vma=False)
```
